32 devices in a mesh: grp: 2 (over y), ep: 4 (over z), tp: 4 (over x, core).
Axes of the slice: x: 2, y: 2, z: 4, core: 2. Of those that a mesh axis runs over, the one named last changes fastest.
Arguments:
- query_vectors: bfloat16 [4096, 2048], P(('grp', 'ep'), 'tp'), parts along dimension 0, may hold values from -6 to 6
- attend_lookup_vectors: bfloat16 [4096, 2048], P(('grp', 'ep'), 'tp'), parts along dimension 0, may hold values from -6 to 6
- attend_content_vectors: bfloat16 [4096, 2048], P(('grp', 'ep'), 'tp'), parts along dimension 0, may hold values from -6 to 6
- forget_speed_dependent: bfloat16 [4096, 2048], P(('grp', 'ep'), 'tp'), parts along dimension 0, may hold values from -3 to 3
- amend_speed_dependent: bfloat16 [4096, 2048], P(('grp', 'ep'), 'tp'), parts along dimension 0, may hold values from -6 to 6
- result_switch_preactivation: bfloat16 [4096, 2048], P(('grp', 'ep'), 'tp'), parts along dimension 0, may hold values from -6 to 6
- feature_forget_baseline: float32 [2048], P('tp'), may hold values from -13 to -3
- amend_speed_baseline: float32 [2048], P('tp'), may hold values from -9 to 3
- sudden_forget_extra: float32 [4096, 32], P(('grp', 'ep'), 'tp'), parts along dimension 0, may hold values from -1 to 0
- group_scaling_factor: float32 [2048], P('tp'), may hold values from 0.1 to 1.9
- result_mapping_matrix: bfloat16 [2048, 2048], P('tp'), may hold values from -0.125 to 0.125
- specialist_tokens_activations: bfloat16 [4096, 2048], P(('grp', 'ep', 'tp')), parts along dimension 0, may hold values from -6 to 6
- specialist_scaling_factor: float32 [2048], replicated, may hold values from 0.1 to 1.9
- selected_specialists: int32 [4096, 2], P(('grp', 'ep', 'tp')), parts along dimension 0, may hold values from 0 to 3, all different within a row; in each aligned block of 128 rows (0 to 127, 128 to 255, ...) at most 96 rows name the same one
- selection_mixing_factors: float32 [4096, 2], P(('grp', 'ep', 'tp')), parts along dimension 0, may hold values from 0.3 to 1.5
- dispatched_switch_matrix: bfloat16 [4, 2048, 1024], P('ep', None, 'tp'), may hold values from -0.125 to 0.125
- dispatched_raising_matrix: bfloat16 [4, 2048, 1024], P('ep', None, 'tp'), may hold values from -0.125 to 0.125
- dispatched_lowering_matrix: bfloat16 [4, 1024, 2048], P('ep', 'tp'), may hold values from -0.1875 to 0.1875
- common_switch_matrix: bfloat16 [2048, 512], P(None, 'tp'), may hold values from -0.125 to 0.125
- common_raising_matrix: bfloat16 [2048, 512], P(None, 'tp'), may hold values from -0.125 to 0.125
- common_lowering_matrix: bfloat16 [512, 2048], P('tp'), may hold values from -0.25 to 0.25
Outputs:
- attend_result_matrix: bfloat16 [4096, 2048], P(('grp', 'ep', 'tp')), parts along dimension 0
- moe_out: bfloat16 [4096, 2048], P(('grp', 'ep', 'tp')), parts along dimension 0
The draws below stay inside these ranges and needn't reach their ends.
There are 2 independent parts, one for each index of `grp`. The reference program is written for one: setup_inputs(seed, part) draws one part's arguments, and reference() takes and returns one part's arrays. A program takes and returns all parts, laid end to end along the dimension named above; an argument that names none is the same for every part. Nothing has to cross between parts.
Inputs may be any that keep to these rules, and one draw needn't show every extreme that they name: `selected_specialists`: each row names 2 different experts. Among the rows of one device no expert is named more than 96 times, and in every draw some device names some expert exactly 96 times.
All inputs are finite; a program needn't handle non-finite values.
Results may differ from the reference program's by a relative error of at most 0.023.
Values may be sent and summed in bfloat16 or wider, within the bound.
A program may use at most 128 MiB of HBM per device.

```python
import math
import jax
import jax.numpy as jnp
import numpy as np
from jax import lax

D = 2048
ATTEND_GROUPS = 32
ATTEND_SIZE = 64
FF = 1024
SFF = 512
TOP = 2
TOK_A = 512
TOK_B = 128
TOKENS_A = 2048
TOKENS_B = 2048
EXPERTS = 4
CAP = 96
N_TP = 4


def slow_heads(key):
    chance = 0.5
    return jax.random.uniform(jax.random.fold_in(key, 101), (ATTEND_GROUPS,), jnp.float32) < chance


def draw_feature_forget_baseline(key, part):
    slow_mask = slow_heads(key)
    spread = jax.random.uniform(jax.random.fold_in(key, 202), (ATTEND_GROUPS, ATTEND_SIZE), jnp.float32)
    slow_log = jnp.log(0.05 / TOKENS_A) + spread * jnp.log(8.0)
    fast_log = jnp.log(0.01) + spread * jnp.log(100.0 / 30.0)
    return jnp.where(slow_mask[:, None], slow_log, fast_log).reshape(ATTEND_GROUPS * ATTEND_SIZE).astype(jnp.float32)


def draw_amend_speed_baseline(key, part):
    slow_mask = slow_heads(key)
    noise = jnp.clip(jax.random.normal(jax.random.fold_in(key, 303), (ATTEND_GROUPS, ATTEND_SIZE), jnp.float32), -3.0, 3.0)
    return jnp.where(slow_mask[:, None], -7.0 + 0.5 * noise, noise).reshape(ATTEND_GROUPS * ATTEND_SIZE).astype(jnp.float32)


def draw_forget_speed_dependent(key, part):
    block_count = TOKENS_A // TOK_A
    offsets = jax.random.uniform(jax.random.fold_in(key, 1), (block_count,), jnp.float32, -0.7, 0.7)
    noise = jnp.clip(0.6 * jax.random.normal(jax.random.fold_in(key, 2), (TOKENS_A, ATTEND_GROUPS * ATTEND_SIZE), jnp.float32), -2.0, 2.0)
    return (noise + jnp.repeat(offsets, TOK_A)[:, None]).astype(jnp.bfloat16)


def draw_sudden_forget_extra(key, part):
    where_at = jax.random.randint(jax.random.fold_in(key, 1), (2, 1, ATTEND_GROUPS), 0, TOKENS_A)
    losses = jax.random.uniform(jax.random.fold_in(key, 2), (2, 1, ATTEND_GROUPS), jnp.float32, jnp.log(0.6), jnp.log(0.8))
    row_ids = jnp.arange(TOKENS_A, dtype=jnp.int32)[None, :, None]
    return jnp.sum(jnp.where(row_ids == where_at, losses, 0.0), axis=0).astype(jnp.float32)


def block_levels(own_key, dims, pieces, low, high):
    level = 1.0
    for axis_at, parts in pieces:
        steps = jax.random.uniform(jax.random.fold_in(jax.random.fold_in(own_key, 6), axis_at), (parts,), jnp.float32, low / len(pieces), high / len(pieces))
        level = level * jnp.repeat(jnp.exp(steps), dims[axis_at] // parts).reshape((-1,) + (1,) * (len(dims) - 1 - axis_at))
    return level


def routed_block(rng, own, number, rows, count, top, reach, lean):
    ranking = jax.random.permutation(rng, count)
    heavy_load, common = load_shares(count, rows * top, reach, lean, True), load_shares(count, rows * top, reach, lean, False)
    places = jnp.arange(count)

    def named(sizes, offset_by):
        used = int((sizes > 0).sum())
        fixed = max(1, used // 4)
        shifted = fixed + (places - fixed + offset_by * (used - fixed)) % max(1, count - fixed)
        return jnp.zeros((count,), jnp.int32).at[ranking[jnp.where(places < fixed, places, shifted)]].set(jnp.asarray(sizes, jnp.int32))

    sizes = jnp.where(number % 4 == 0, named(heavy_load, number // 4), named(common, number - number // 4 - 1))
    mixed = jax.random.permutation(jax.random.fold_in(own, 3), count)
    source_of, receiver = mixed[0:count // 2 * 2:2], mixed[1:count // 2 * 2:2]
    room = jnp.minimum(sizes[source_of] - 1, reach - sizes[receiver]) // 2
    room = jnp.where((source_of == ranking[0]) | (receiver == ranking[0]) | (sizes[receiver] == 0), 0, jnp.maximum(room, 0))
    shifted = jax.random.randint(jax.random.fold_in(own, 4), (count // 2,), 0, 1 << 20) % (room + 1)
    sizes = sizes.at[source_of].add(-shifted).at[receiver].add(shifted)
    items = jnp.searchsorted(jnp.cumsum(sizes), jnp.arange(rows * top), side="right").astype(jnp.int32)
    table = items.reshape(top, rows).T
    table = table[jax.random.permutation(jax.random.fold_in(own, 1), rows)]
    offset_by = jax.random.randint(jax.random.fold_in(own, 2), (rows, 1), 0, top)
    return jnp.take_along_axis(table, (jnp.arange(top)[None, :] + offset_by) % top, axis=1)


def load_shares(number_of, total, bound, skew, full):
    loads = [(1 << 20) // math.isqrt(standing ** skew) + 1 for standing in range(1, number_of + 1)]
    largest = bound if full else min(bound, max(-(-total // number_of), total * loads[0] // sum(loads)))
    least = 1 if total - largest >= number_of - 1 else 0
    given, rest = [largest] + [least] * (number_of - 1), total - largest - least * (number_of - 1)
    while rest > 0:
        candidates = [i for i in range(1, number_of) if given[i] < largest] or [i for i in range(1, number_of) if given[i] < bound]
        mass, left = sum([loads[i] for i in candidates]), rest
        for i in candidates:
            extra = min(bound - given[i], max(1, left * loads[i] // mass), rest)
            given[i] = given[i] + extra
            rest = rest - extra
    return np.array(given)


def centred(rng, dims, width, reach, shards=(), kind=jnp.bfloat16):
    level = block_levels(rng, dims, shards, -0.22, 0.18) if shards else 1.0
    result = jax.random.normal(rng, dims, jnp.float32) * width * level
    return jnp.minimum(jnp.maximum(result, -reach), reach).astype(kind)


def setup_inputs(seed: int = 0, part: int = 0) -> dict:
    arg_keys = jax.random.split(jax.random.key(seed), 22)
    part_splits = jax.random.split(jax.random.fold_in(arg_keys[21], part), 22)
    query_vectors = centred(part_splits[0], (TOKENS_A, ATTEND_GROUPS * ATTEND_SIZE), 1.0, 6.0, ((0, 4), (1, 4)))
    attend_lookup_vectors = centred(part_splits[1], (TOKENS_A, ATTEND_GROUPS * ATTEND_SIZE), 1.0, 6.0, ((0, 4), (1, 4)))
    attend_content_vectors = centred(part_splits[2], (TOKENS_A, ATTEND_GROUPS * ATTEND_SIZE), 1.0, 6.0, ((0, 4), (1, 4)))
    forget_speed_dependent = draw_forget_speed_dependent(jax.random.fold_in(jax.random.fold_in(arg_keys[21], part), 71), part)
    amend_speed_dependent = centred(part_splits[4], (TOKENS_A, ATTEND_GROUPS * ATTEND_SIZE), 1.0, 6.0, ((0, 4), (1, 4)))
    result_switch_preactivation = centred(part_splits[5], (TOKENS_A, ATTEND_GROUPS * ATTEND_SIZE), 1.0, 6.0, ((0, 4), (1, 4)))
    feature_forget_baseline = draw_feature_forget_baseline(jax.random.fold_in(arg_keys[21], 71), part)
    amend_speed_baseline = draw_amend_speed_baseline(jax.random.fold_in(arg_keys[21], 71), part)
    sudden_forget_extra = draw_sudden_forget_extra(jax.random.fold_in(jax.random.fold_in(arg_keys[21], part), 71), part)
    group_scaling_factor = jnp.clip(1.0 + 0.18 * jax.random.normal(arg_keys[9], (ATTEND_GROUPS * ATTEND_SIZE,), jnp.float32), 0.1, 1.9)
    result_mapping_matrix = centred(arg_keys[10], (ATTEND_GROUPS * ATTEND_SIZE, D), (ATTEND_GROUPS * ATTEND_SIZE) ** -0.5, 0.125, ((0, 4),))
    specialist_tokens_activations = centred(part_splits[11], (TOKENS_B, D), 1.0, 6.0, ((0, 16),))
    specialist_scaling_factor = jnp.clip(1.0 + 0.18 * jax.random.normal(arg_keys[12], (D,), jnp.float32), 0.1, 1.9)
    selected_specialists_keys = jax.random.split(jax.random.fold_in(part_splits[13], 1), TOKENS_B // TOK_B)
    selected_specialists_turns = jax.random.permutation(jax.random.fold_in(part_splits[13], 3), TOKENS_B // TOK_B)
    selected_specialists = jax.vmap(lambda own, number: routed_block(jax.random.fold_in(part_splits[13], 2), own, number, TOK_B, EXPERTS, TOP, CAP, 2))(selected_specialists_keys, selected_specialists_turns).reshape((TOKENS_B, TOP))
    selection_mixing_factors = jnp.clip(jnp.exp(math.log(1.5) - 1.60943787 * jax.random.uniform(part_splits[14], (TOKENS_B, TOP), jnp.float32) ** block_levels(part_splits[14], (TOKENS_B, TOP), ((0, 16),), -0.2, 0.2)), 0.3, 1.5)
    dispatched_switch_matrix = centred(arg_keys[15], (EXPERTS, D, FF), D ** -0.5, 0.125, ((0, 4), (2, 4)))
    dispatched_raising_matrix = centred(arg_keys[16], (EXPERTS, D, FF), D ** -0.5, 0.125, ((0, 4), (2, 4)))
    dispatched_lowering_matrix = centred(arg_keys[17], (EXPERTS, FF, D), FF ** -0.5, 0.1875, ((0, 4), (1, 4)))
    common_switch_matrix = centred(arg_keys[18], (D, SFF), D ** -0.5, 0.125, ((1, 4),))
    common_raising_matrix = centred(arg_keys[19], (D, SFF), D ** -0.5, 0.125, ((1, 4),))
    common_lowering_matrix = centred(arg_keys[20], (SFF, D), SFF ** -0.5, 0.25, ((0, 4),))
    return dict(query_vectors=query_vectors, attend_lookup_vectors=attend_lookup_vectors, attend_content_vectors=attend_content_vectors, forget_speed_dependent=forget_speed_dependent, amend_speed_dependent=amend_speed_dependent, result_switch_preactivation=result_switch_preactivation, feature_forget_baseline=feature_forget_baseline, amend_speed_baseline=amend_speed_baseline, sudden_forget_extra=sudden_forget_extra, group_scaling_factor=group_scaling_factor, result_mapping_matrix=result_mapping_matrix, specialist_tokens_activations=specialist_tokens_activations, specialist_scaling_factor=specialist_scaling_factor, selected_specialists=selected_specialists, selection_mixing_factors=selection_mixing_factors, dispatched_switch_matrix=dispatched_switch_matrix, dispatched_raising_matrix=dispatched_raising_matrix, dispatched_lowering_matrix=dispatched_lowering_matrix, common_switch_matrix=common_switch_matrix, common_raising_matrix=common_raising_matrix, common_lowering_matrix=common_lowering_matrix)


highest = lax.Precision.HIGHEST

def split_sum(hidden, weight, blocks):
    width_dev = hidden.shape[1] // blocks
    summed = jnp.zeros((hidden.shape[0], weight.shape[1]), jnp.float32)
    for block_id in range(blocks):
        lower = block_id * width_dev
        partial_value = jnp.dot(hidden[:, lower:lower + width_dev], weight[lower:lower + width_dev], preferred_element_type=jnp.float32)
        summed = summed + lax.optimization_barrier(partial_value.astype(jnp.bfloat16)).astype(jnp.float32)
    return summed

def swiglu_rows(rows, gate_w, up_w):
    gate_vals = jnp.dot(rows, gate_w, preferred_element_type=jnp.float32)
    up_vals = jnp.dot(rows, up_w, preferred_element_type=jnp.float32)
    return (jax.nn.silu(gate_vals) * up_vals).astype(jnp.bfloat16)

def simple_attend_verify(query_vectors, attend_lookup_vectors, attend_content_vectors, forget_speed_dependent, amend_speed_dependent, result_switch_preactivation, feature_forget_baseline, amend_speed_baseline, sudden_forget_extra, group_scaling_factor, result_mapping_matrix):
    tokens = query_vectors.shape[0]

    def split_among_groups(array_in):
        return array_in.astype(jnp.float32).reshape(tokens, ATTEND_GROUPS, ATTEND_SIZE)
    forget_exponent_log = -jnp.exp(feature_forget_baseline.reshape(ATTEND_GROUPS, ATTEND_SIZE) + split_among_groups(forget_speed_dependent)) + sudden_forget_extra[:, :, None]
    learn_rate = jax.nn.sigmoid(amend_speed_baseline.reshape(ATTEND_GROUPS, ATTEND_SIZE) + split_among_groups(amend_speed_dependent))
    key_heads = split_among_groups(attend_lookup_vectors)
    unit_key = key_heads * lax.rsqrt(lax.optimization_barrier(jnp.sum(key_heads * key_heads, -1, keepdims=True)) + 1e-06)

    def advance(memory, inputs):
        recept_now, decay_now, write_now, value_now, unit_now, erase_now = inputs
        removed = jnp.einsum('hvk,hk->hv', memory, -unit_now, precision=highest)
        memory = memory * decay_now[:, None, :] + removed[:, :, None] * erase_now[:, None, :] + value_now[:, :, None] * write_now[:, None, :]
        return (memory, jnp.einsum('hvk,hk->hv', memory, recept_now, precision=highest))
    memory_zero = jnp.zeros((ATTEND_GROUPS, ATTEND_SIZE, ATTEND_SIZE), jnp.float32)
    memory_end, recur = lax.scan(advance, memory_zero, (split_among_groups(query_vectors), jnp.exp(forget_exponent_log), key_heads * learn_rate, split_among_groups(attend_content_vectors), unit_key, unit_key * learn_rate))
    head_mean = lax.optimization_barrier(jnp.mean(recur, -1, keepdims=True))
    centered = recur - head_mean
    head_var = lax.optimization_barrier(jnp.mean(centered * centered, -1, keepdims=True))
    normed = centered * lax.rsqrt(head_var + 0.00064) * group_scaling_factor.reshape(ATTEND_GROUPS, ATTEND_SIZE)
    mixed_rows = (normed * jax.nn.sigmoid(split_among_groups(result_switch_preactivation))).reshape(tokens, ATTEND_GROUPS * ATTEND_SIZE)
    mixed_rows = mixed_rows.astype(jnp.bfloat16)
    return split_sum(mixed_rows, result_mapping_matrix, N_TP).astype(jnp.bfloat16)

def moe_reference(specialist_tokens_activations, specialist_scaling_factor, selected_specialists, selection_mixing_factors, dispatched_switch_matrix, dispatched_raising_matrix, dispatched_lowering_matrix, common_switch_matrix, common_raising_matrix, common_lowering_matrix):
    floats = specialist_tokens_activations.astype(jnp.float32)
    normed = floats * lax.rsqrt(lax.optimization_barrier(jnp.mean(floats * floats, -1, keepdims=True)) + 1e-06) * specialist_scaling_factor
    normed = normed.astype(jnp.bfloat16)
    top_count = selected_specialists.shape[1]
    block_count = TOKENS_B // TOK_B
    flat_block = selected_specialists.reshape(block_count, TOK_B * top_count)
    one_hot = (flat_block[:, :, None] == jnp.arange(EXPERTS, dtype=jnp.int32)[None, None, :]).astype(jnp.int32)
    slot_rank = lax.optimization_barrier(jnp.sum((jnp.cumsum(one_hot, axis=1) - 1) * one_hot, axis=-1))
    position = (jnp.arange(block_count, dtype=jnp.int32)[:, None] * CAP + slot_rank).reshape(-1)
    flat_ids = flat_block.reshape(-1)
    weights_flat = selection_mixing_factors.reshape(-1)
    repeated = jnp.repeat(normed, top_count, axis=0)
    buffer_rows = block_count * CAP

    def per_expert(summed, operands):
        gate_w, up_w, down_w, expert_id = operands
        chosen = flat_ids == expert_id
        target = jnp.where(chosen, position, buffer_rows)
        buffer = jnp.zeros((buffer_rows, D), jnp.bfloat16).at[target].set(repeated, mode='drop')
        hidden = swiglu_rows(buffer, gate_w, up_w)
        expert_out = split_sum(hidden, down_w, N_TP).astype(jnp.bfloat16)
        picked = jnp.take(expert_out, jnp.minimum(position, buffer_rows - 1), axis=0).astype(jnp.float32)
        contrib = jnp.where(chosen[:, None], picked * weights_flat[:, None], 0.0)
        return (summed + lax.optimization_barrier(jnp.sum(contrib.reshape(TOKENS_B, top_count, D), axis=1)), None)
    routed, _ = lax.scan(per_expert, jnp.zeros((TOKENS_B, D), jnp.float32), (dispatched_switch_matrix, dispatched_raising_matrix, dispatched_lowering_matrix, jnp.arange(EXPERTS, dtype=jnp.int32)))
    shared_hidden = swiglu_rows(normed, common_switch_matrix, common_raising_matrix)
    shared_sum = split_sum(shared_hidden, common_lowering_matrix, N_TP)
    return (routed + shared_sum).astype(jnp.bfloat16)

def reference(query_vectors, attend_lookup_vectors, attend_content_vectors, forget_speed_dependent, amend_speed_dependent, result_switch_preactivation, feature_forget_baseline, amend_speed_baseline, sudden_forget_extra, group_scaling_factor, result_mapping_matrix, specialist_tokens_activations, specialist_scaling_factor, selected_specialists, selection_mixing_factors, dispatched_switch_matrix, dispatched_raising_matrix, dispatched_lowering_matrix, common_switch_matrix, common_raising_matrix, common_lowering_matrix):
    attend_result_matrix = simple_attend_verify(query_vectors, attend_lookup_vectors, attend_content_vectors, forget_speed_dependent, amend_speed_dependent, result_switch_preactivation, feature_forget_baseline, amend_speed_baseline, sudden_forget_extra, group_scaling_factor, result_mapping_matrix)
    moe_out = moe_reference(specialist_tokens_activations, specialist_scaling_factor, selected_specialists, selection_mixing_factors, dispatched_switch_matrix, dispatched_raising_matrix, dispatched_lowering_matrix, common_switch_matrix, common_raising_matrix, common_lowering_matrix)
    return (attend_result_matrix, moe_out)
```

```python
import functools
import math

import jax
import jax.numpy as jnp
from jax import lax
from jax.experimental import pallas as pl
from jax.experimental.pallas import tpu as pltpu
from jax.sharding import PartitionSpec as P

highest = lax.Precision.HIGHEST


NN = (((1,), (0,)), ((), ()))
NT = (((1,), (1,)), ((), ()))


def split_two(array_in):
    high = array_in.astype(jnp.bfloat16)
    return high, (array_in - high.astype(jnp.float32)).astype(jnp.bfloat16)


def dot_parts(left, right, dims):
    def one(x, y):
        return lax.dot_general(x, y, dims, preferred_element_type=jnp.float32)

    return one(left[0], right[0]) + (one(left[0], right[1]) + one(left[1], right[0]))


def dot3(left, right, dims=NN):
    return dot_parts(split_two(left), split_two(right), dims)


def span_kernel(
    heads, size, q_ref, k_ref, v_ref, f_ref, a_ref, fb_ref, ab_ref, extra_ref, out_ref, memory_ref
):
    span = q_ref.shape[0]

    @pl.when(pl.program_id(0) == 0)
    def _():
        row = lax.broadcasted_iota(jnp.int32, (2 * size, size), 0)
        col = lax.broadcasted_iota(jnp.int32, (2 * size, size), 1)
        start = jnp.where(row == col + size, 1.0, 0.0)
        for h in range(heads):
            memory_ref[h] = start

    row = lax.broadcasted_iota(jnp.int32, (span, span), 0)
    col = lax.broadcasted_iota(jnp.int32, (span, span), 1)
    eye = jnp.where(row == col, 1.0, 0.0)
    below = jnp.where(row >= col, 1.0, 0.0)
    row2 = lax.broadcasted_iota(jnp.int32, (2 * span, 2 * span), 0)
    col2 = lax.broadcasted_iota(jnp.int32, (2 * span, 2 * span), 1)
    col2 = jnp.where(col2 >= span, col2 - span, col2)
    pair_mask = jnp.where(row2 >= span, row2 - span + 1, row2) > col2
    levels = []
    width = 1
    while width < span:
        levels.append(
            (row // (2 * width) == col // (2 * width))
            & (row // width % 2 == 1)
            & (col // width % 2 == 0)
        )
        width *= 2

    q_all = q_ref[...].astype(jnp.float32)
    k_all = k_ref[...].astype(jnp.float32)
    v_all = v_ref[...].astype(jnp.float32)
    rate_all = jax.nn.sigmoid(ab_ref[...] + a_ref[...].astype(jnp.float32))
    speed = -jnp.exp(fb_ref[...] + f_ref[...].astype(jnp.float32))
    extra = extra_ref[...]
    decay_all = speed + jnp.concatenate(
        [jnp.broadcast_to(extra[:, h : h + 1], (span, size)) for h in range(heads)], axis=1
    )
    cum_all = jnp.dot(below, decay_all, precision=highest, preferred_element_type=jnp.float32)
    prev_all = cum_all - decay_all
    middle = cum_all[span // 2 : span // 2 + 1]
    last = cum_all[span - 1 : span]
    exp_prev_mid = jnp.exp(prev_all - middle)
    exp_cum_mid = jnp.exp(cum_all - middle)
    exp_mid_cum = jnp.exp(middle - cum_all)
    exp_prev = jnp.exp(prev_all)
    exp_cum = jnp.exp(cum_all)
    exp_tail = jnp.exp(last - cum_all)
    exp_last = jnp.exp(last)
    write_all = k_all * rate_all
    squares = k_all * k_all

    every = range(heads)

    def cut(array_in, h):
        return array_in[:, h * size : (h + 1) * size]

    norms = [lax.rsqrt(jnp.sum(cut(squares, h), -1, keepdims=True) + 1e-06) for h in every]
    unit_all = k_all * jnp.concatenate(
        [jnp.broadcast_to(n, (span, size)) for n in norms], axis=1
    )
    erase_all = unit_all * rate_all
    left_all = jnp.concatenate([-unit_all * exp_prev_mid, q_all * exp_cum_mid], axis=0)
    right_all = jnp.concatenate([erase_all * exp_mid_cum, write_all * exp_mid_cum], axis=0)
    read_all = jnp.concatenate([-unit_all * exp_prev, q_all * exp_cum], axis=0)
    tail_all = jnp.concatenate([erase_all * exp_tail, write_all * exp_tail], axis=0)
    left_all, right_all = split_two(left_all), split_two(right_all)
    read_all, tail_all = split_two(read_all), split_two(tail_all)

    def cut2(parts, h):
        return tuple(cut(part, h) for part in parts)

    pairs = [
        jnp.where(pair_mask, dot_parts(cut2(left_all, h), cut2(right_all, h), NT), 0.0)
        for h in every
    ]
    strict = [p[:span, :span] for p in pairs]
    solved = [eye + jnp.where(levels[0], s, 0.0) for s in strict]
    for level in levels[1:]:
        halves = [split_two(x) for x in solved]
        middles = [
            dot_parts(split_two(jnp.where(level, s, 0.0)), x, NN) for s, x in zip(strict, halves)
        ]
        solved = [
            x + dot_parts(xs, split_two(m), NN) for x, xs, m in zip(solved, halves, middles)
        ]
    memories = [memory_ref[h] for h in every]
    reads = [dot_parts(cut2(read_all, h), split_two(memories[h]), NT) for h in every]
    blank = jnp.zeros((span, size), jnp.float32)
    values = [jnp.concatenate([cut(v_all, h), blank], axis=1) for h in every]
    rights = [
        reads[h][:span] + dot3(pairs[h][:span, span:], values[h]) for h in every
    ]
    updates = [dot3(solved[h], rights[h]) for h in every]
    stacked = [jnp.concatenate([updates[h], values[h]], axis=0) for h in every]
    for h in every:
        out_ref[:, 2 * size * h : 2 * size * (h + 1)] = reads[h][span:] + dot3(
            pairs[h][span:], stacked[h]
        )
    for h in every:
        memory_ref[h] = memories[h] * cut(exp_last, h) + dot_parts(
            split_two(stacked[h].T), cut2(tail_all, h), NN
        )


def finish_kernel(
    heads, size, place_ref, parts_ref, flat_ref, gate_ref, gain_ref, mixed_ref, state_ref
):
    @pl.when(pl.program_id(0) == 0)
    def _():
        state_ref[...] = jnp.zeros_like(state_ref)

        @pl.loop(0, place_ref[0])
        def _(k):
            for h in range(heads):
                part = parts_ref[k, h]
                own = split_two(state_ref[h])
                carry = part[size:]
                moved = lax.dot_general(
                    own[0], carry, NN, preferred_element_type=jnp.float32
                ) + lax.dot_general(own[1], carry, NN, preferred_element_type=jnp.float32)
                state_ref[h] = moved + part[:size].astype(jnp.float32)

    centered_all = []
    for h in range(heads):
        flat = flat_ref[:, 2 * size * h : 2 * size * (h + 1)]
        head_out = flat[:, :size] + dot3(flat[:, size:], state_ref[h], NT)
        centered = head_out - jnp.mean(head_out, -1, keepdims=True)
        head_var = jnp.mean(centered * centered, -1, keepdims=True)
        centered_all.append(centered * lax.rsqrt(head_var + 0.00064))
    scaled = jnp.concatenate(centered_all, axis=1) * gain_ref[...]
    gate = jax.nn.sigmoid(gate_ref[...].astype(jnp.float32))
    mixed_ref[...] = (scaled * gate).astype(jnp.bfloat16)


def mixer_half(
    query_vectors,
    attend_lookup_vectors,
    attend_content_vectors,
    forget_speed_dependent,
    amend_speed_dependent,
    result_switch_preactivation,
    feature_forget_baseline,
    amend_speed_baseline,
    sudden_forget_extra,
    group_scaling_factor,
):
    tokens, mix_width = query_vectors.shape
    heads = sudden_forget_extra.shape[1]
    size = mix_width // heads
    span = math.gcd(tokens, 64)
    rows = pl.BlockSpec((span, mix_width), lambda i: (i, 0))
    whole_row = pl.BlockSpec((1, mix_width), lambda i: (0, 0))
    wide = pl.BlockSpec((span, 2 * mix_width), lambda i: (i, 0))
    serial = pltpu.CompilerParams(dimension_semantics=("arbitrary",))
    flat_out, memory_end = pl.pallas_call(
        functools.partial(span_kernel, heads, size),
        grid=(tokens // span,),
        in_specs=[
            rows,
            rows,
            rows,
            rows,
            rows,
            whole_row,
            whole_row,
            pl.BlockSpec((span, heads), lambda i: (i, 0)),
        ],
        out_specs=[wide, pl.BlockSpec((heads, 2 * size, size), lambda i: (0, 0, 0))],
        out_shape=[
            jax.ShapeDtypeStruct((tokens, 2 * mix_width), jnp.float32),
            jax.ShapeDtypeStruct((heads, 2 * size, size), jnp.float32),
        ],
        compiler_params=serial,
        cost_estimate=pl.CostEstimate(
            flops=100_000_000_000 // 2, bytes_accessed=5_000_000, transcendentals=0
        ),
        name="spans",
    )(
        query_vectors,
        attend_lookup_vectors,
        attend_content_vectors,
        forget_speed_dependent,
        amend_speed_dependent,
        feature_forget_baseline.reshape(1, mix_width),
        amend_speed_baseline.reshape(1, mix_width),
        sudden_forget_extra,
    )
    parts = lax.all_gather(memory_end.astype(jnp.bfloat16), "ep")
    place = lax.axis_index("ep").reshape(1).astype(jnp.int32)
    return pl.pallas_call(
        functools.partial(finish_kernel, heads, size),
        grid=(tokens // span,),
        in_specs=[
            pl.BlockSpec(memory_space=pltpu.SMEM),
            pl.BlockSpec(parts.shape, lambda i: (0, 0, 0, 0)),
            wide,
            rows,
            whole_row,
        ],
        out_specs=rows,
        out_shape=jax.ShapeDtypeStruct((tokens, mix_width), jnp.bfloat16),
        scratch_shapes=[pltpu.VMEM((heads, size, size), jnp.float32)],
        compiler_params=serial,
        cost_estimate=pl.CostEstimate(
            flops=10_000_000_000, bytes_accessed=4_000_000, transcendentals=0
        ),
        name="finish",
    )(
        place,
        parts,
        flat_out,
        result_switch_preactivation,
        group_scaling_factor.reshape(1, mix_width),
    )


def swiglu_rows(rows, gate_w, up_w):
    gate_vals = jnp.dot(rows, gate_w, preferred_element_type=jnp.float32)
    up_vals = jnp.dot(rows, up_w, preferred_element_type=jnp.float32)
    return (jax.nn.silu(gate_vals) * up_vals).astype(jnp.bfloat16)


def on_device(
    query_vectors,
    attend_lookup_vectors,
    attend_content_vectors,
    forget_speed_dependent,
    amend_speed_dependent,
    result_switch_preactivation,
    feature_forget_baseline,
    amend_speed_baseline,
    sudden_forget_extra,
    group_scaling_factor,
    result_mapping_matrix,
    specialist_tokens_activations,
    specialist_scaling_factor,
    selected_specialists,
    selection_mixing_factors,
    dispatched_switch_matrix,
    dispatched_raising_matrix,
    dispatched_lowering_matrix,
    common_switch_matrix,
    common_raising_matrix,
    common_lowering_matrix,
):
    mixed_rows = mixer_half(
        query_vectors,
        attend_lookup_vectors,
        attend_content_vectors,
        forget_speed_dependent,
        amend_speed_dependent,
        result_switch_preactivation,
        feature_forget_baseline,
        amend_speed_baseline,
        sudden_forget_extra,
        group_scaling_factor,
    )
    floats = specialist_tokens_activations.astype(jnp.float32)
    normed = (
        floats
        * lax.rsqrt(jnp.mean(floats * floats, -1, keepdims=True) + 1e-06)
        * specialist_scaling_factor
    )
    normed = normed.astype(jnp.bfloat16)
    tok_rows, top_count = selected_specialists.shape
    model_width = specialist_tokens_activations.shape[1]
    experts = lax.axis_size("ep")
    capacity = 3 * tok_rows * top_count // (2 * experts)
    flat_ids = selected_specialists.reshape(-1)
    one_hot = (flat_ids[:, None] == jnp.arange(experts, dtype=jnp.int32)[None, :]).astype(jnp.int32)
    slot_rank = jnp.sum((jnp.cumsum(one_hot, axis=0) - 1) * one_hot, axis=1)
    position = flat_ids * capacity + slot_rank
    placing = position[:, None] == jnp.arange(experts * capacity, dtype=jnp.int32)[None, :]
    placing = jnp.sum(
        placing.astype(jnp.bfloat16).reshape(tok_rows, top_count, experts * capacity), axis=1
    )
    outgoing = jnp.einsum("te,td->ed", placing, normed, preferred_element_type=jnp.float32).astype(
        jnp.bfloat16
    )
    gate_w = dispatched_switch_matrix[0]
    up_w = dispatched_raising_matrix[0]
    down_w = dispatched_lowering_matrix[0]
    received = lax.all_to_all(
        outgoing.reshape(experts, capacity, model_width),
        "ep",
        split_axis=0,
        concat_axis=0,
        tiled=True,
    )
    local_rows = experts * capacity
    hidden = swiglu_rows(
        lax.all_gather(received.reshape(local_rows, model_width), "tp", axis=0, tiled=True),
        gate_w,
        up_w,
    )
    summed = lax.psum_scatter(
        jnp.dot(hidden, down_w, preferred_element_type=jnp.float32).astype(jnp.bfloat16),
        "tp",
        scatter_dimension=0,
        tiled=True,
    )
    expert_out = lax.all_to_all(
        summed.reshape(experts, capacity, model_width),
        "ep",
        split_axis=0,
        concat_axis=0,
        tiled=True,
    ).reshape(experts * capacity, model_width)
    picked = jnp.take(expert_out, position, axis=0).astype(jnp.float32)
    routed = jnp.sum(
        (picked * selection_mixing_factors.reshape(-1)[:, None]).reshape(
            tok_rows, top_count, model_width
        ),
        axis=1,
    )
    shared_hidden = swiglu_rows(
        lax.all_gather(normed, "tp", axis=0, tiled=True),
        common_switch_matrix,
        common_raising_matrix,
    )
    attend_result_matrix = lax.psum_scatter(
        jnp.dot(mixed_rows, result_mapping_matrix, preferred_element_type=jnp.float32).astype(
            jnp.bfloat16
        ),
        "tp",
        scatter_dimension=0,
        tiled=True,
    )
    shared_sum = lax.psum_scatter(
        jnp.dot(shared_hidden, common_lowering_matrix, preferred_element_type=jnp.float32).astype(
            jnp.bfloat16
        ),
        "tp",
        scatter_dimension=0,
        tiled=True,
    ).astype(jnp.float32)
    moe_out = (routed + shared_sum).astype(jnp.bfloat16)
    return (attend_result_matrix, moe_out)


def solution(mesh):
    placed = (
        P(("grp", "ep"), "tp"),
        P(("grp", "ep"), "tp"),
        P(("grp", "ep"), "tp"),
        P(("grp", "ep"), "tp"),
        P(("grp", "ep"), "tp"),
        P(("grp", "ep"), "tp"),
        P("tp"),
        P("tp"),
        P(("grp", "ep"), "tp"),
        P("tp"),
        P("tp", None),
        P(("grp", "ep", "tp"), None),
        P(),
        P(("grp", "ep", "tp"), None),
        P(("grp", "ep", "tp"), None),
        P("ep", None, "tp"),
        P("ep", None, "tp"),
        P("ep", "tp", None),
        P(None, "tp"),
        P(None, "tp"),
        P("tp", None),
    )
    return jax.shard_map(
        on_device,
        mesh=mesh,
        in_specs=placed,
        out_specs=(P(("grp", "ep", "tp"), None), P(("grp", "ep", "tp"), None)),
        check_vma=False,
    )
```
